256 devices in a mesh: sp: 16 (over y, x), tp: 16 (over z, core).
Axes of the slice: x: 4, y: 4, z: 8, core: 2. Of those that a mesh axis runs over, the one named last changes fastest.
Arguments:
- query_vectors: bfloat16 [16384, 16, 128], P('sp', 'tp'), may hold values from -6 to 6
- key_vectors: bfloat16 [16384, 16, 128], P('sp', 'tp'), may hold values from -6 to 6
- value_vectors: bfloat16 [16384, 16, 128], P('sp', 'tp'), may hold values from -6 to 6
- out_gate: bfloat16 [16384, 16, 128], P('sp', 'tp'), may hold values from -6 to 6
- decay_rate: float32 [2, 16], P(None, 'tp'), may hold values from 0 to 1
- decay_pre: float32 [2, 16, 16384], P(None, 'tp', 'sp'), may hold values from -6 to 6
- decay_shock: float32 [2, 16, 16384], P(None, 'tp', 'sp'), may hold values from -2 to 0
- beta_pre: float32 [2, 16, 16384], P(None, 'tp', 'sp'), may hold values from -12 to 0
- head_gain: float32 [128], replicated, may hold values from 0.1 to 1.9
- w_out: bfloat16 [2048, 2048], P('tp'), may hold values from -0.125 to 0.125
- tokens: bfloat16 [16384, 2048], P(('sp', 'tp')), may hold values from -6 to 6
- norm_gain: float32 [2048], replicated, may hold values from 0.1 to 1.9
- experts_pick: int32 [16384, 2], P(('sp', 'tp')), may hold values from 0 to 15, as said below
- pair_logits: float32 [16384, 2], P(('sp', 'tp')), may hold values from -6 to 6
- group_logits: float32 [16384, 8], P(('sp', 'tp')), may hold values from -6 to 6
- expert_gate: bfloat16 [16, 2048, 2048], P('sp', None, 'tp'), may hold values from -0.125 to 0.125
- expert_up: bfloat16 [16, 2048, 2048], P('sp', None, 'tp'), may hold values from -0.125 to 0.125
- expert_down: bfloat16 [16, 2048, 2048], P('sp', None, 'tp'), may hold values from -0.5 to 0.5
Outputs:
- layer_out: bfloat16 [16384, 2048], P(('sp', 'tp'))
The draws below stay inside these ranges and needn't reach their ends.
Inputs may be any that keep to these rules, and one draw needn't show every extreme that they name: `experts_pick`: each token names two different experts of one group of 2 consecutive experts. The 64 tokens of one device fall 8 into each group. At most 8 tokens of one device name any one expert, and in every draw every expert is named by 8 tokens of every device.
All inputs are finite; a program needn't handle non-finite values.
Results may differ from the reference program's by a relative error of at most 0.02.
Values may be sent and summed in bfloat16 or wider, within the bound.
No kernel may reach another device: no remote copies, remote signals or barrier semaphores. Data moves between devices by JAX's collectives and lax.ppermute only.
A program may use at most 128 MiB of HBM per device.

```python
import jax
import jax.numpy as jnp
from jax import lax

D = 2048
HEADS = 16
HEAD_DIM = 128
BLOCK = 64
EXP_FF = 2048
GROUP_SIZE = 2
TOK_SP = 1024
SEQ = 16384
TOK_DEV = 64
EXPERTS = 16
EXPERT_GROUPS = 8
CAP = 8
N_TP = 16


def draw_decay_rate(key, part):
    pick_key, slow_key, fast_key = jax.random.split(key, 3)
    chance = jax.random.uniform(pick_key, (2, HEADS), jnp.float32)
    slow_mask = chance < 0.5
    slow_rate = jnp.exp(jax.random.uniform(slow_key, (2, HEADS), jnp.float32, jnp.log(0.15), jnp.log(0.6))) / SEQ
    fast_rate = jnp.exp(jax.random.uniform(fast_key, (2, HEADS), jnp.float32, jnp.log(0.03), jnp.log(0.08)))
    return jnp.where(slow_mask, slow_rate, fast_rate).astype(jnp.float32)


def draw_decay_pre(key, part):
    noise_key, level_key = jax.random.split(key)
    block_count = SEQ // TOK_SP
    ranking = jax.random.permutation(level_key, block_count).astype(jnp.float32)
    levels = -1.5 + 3.0 * ranking / max(block_count - 1, 1)
    noise = jax.random.normal(noise_key, (2, HEADS, block_count, TOK_SP), jnp.float32)
    values_out = jnp.clip(noise + levels[None, None, :, None], -6.0, 6.0)
    return values_out.reshape(2, HEADS, SEQ).astype(jnp.float32)


def draw_decay_shock(key, part):
    place_key, size_key = jax.random.split(key)
    spots = jax.random.randint(place_key, (2, 2), 0, SEQ)
    amounts = jax.random.uniform(size_key, (2, HEADS, 2), jnp.float32, -0.69, -0.22)
    positions = jnp.arange(SEQ)
    marked = (positions[None, None, :] == spots[:, :, None]).astype(jnp.float32)
    return jnp.einsum('dhs,dst->dht', amounts, marked).astype(jnp.float32)


def draw_beta_pre(key, part):
    level_key, noise_key = jax.random.split(jax.random.fold_in(key, 11))
    chain_loss = jnp.exp(jax.random.uniform(level_key, (2, HEADS), jnp.float32, jnp.log(0.3), jnp.log(2.0)))
    target = chain_loss * HEAD_DIM / (2.0 * SEQ)
    level = jnp.log(target) - jnp.log1p(-target) - 0.5
    noise = jnp.clip(jax.random.normal(noise_key, (2, HEADS, SEQ), jnp.float32), -4.0, 4.0)
    return jnp.clip(level[:, :, None] + noise, -12.0, 0.0).astype(jnp.float32)


def draw_experts_pick(key, part):
    block_count = SEQ // TOK_DEV
    group_share = TOK_DEV // EXPERT_GROUPS
    order_key, swap_key = jax.random.split(key)
    ranking = jax.vmap(lambda sub_key: jax.random.permutation(sub_key, TOK_DEV))(jax.random.split(order_key, block_count))
    group_of = ranking // group_share
    swap_bits = jax.random.randint(swap_key, (block_count, TOK_DEV), 0, 2)
    group_base = group_of * GROUP_SIZE
    picks = jnp.stack([group_base + swap_bits, group_base + 1 - swap_bits], axis=-1)
    return picks.reshape(SEQ, 2).astype(jnp.int32)


def block_scale(key, shape, cuts, least, top_value):
    loudness = 1.0
    for dim, blocks in cuts:
        steps = jax.random.uniform(jax.random.fold_in(jax.random.fold_in(key, 6), dim), (blocks,), jnp.float32, least / len(cuts), top_value / len(cuts))
        loudness = loudness * jnp.repeat(jnp.exp(steps), shape[dim] // blocks).reshape((-1,) + (1,) * (len(shape) - 1 - dim))
    return loudness


def gaussian(key, shape, deviation, limit, cuts=(), kind=jnp.bfloat16):
    array = deviation * jax.random.normal(key, shape, jnp.float32)
    if cuts:
        array = array * block_scale(key, shape, cuts, -0.22, 0.18)
    return jnp.clip(array, -limit, limit).astype(kind)


def setup_inputs(seed: int = 0) -> dict:
    splits = jax.random.split(jax.random.key(seed), 19)
    return {
        "query_vectors": gaussian(splits[0], (SEQ, HEADS, HEAD_DIM), 1.0, 6.0, ((0, 16), (1, 16))),
        "key_vectors": gaussian(splits[1], (SEQ, HEADS, HEAD_DIM), 1.0, 6.0, ((0, 16), (1, 16))),
        "value_vectors": gaussian(splits[2], (SEQ, HEADS, HEAD_DIM), 1.0, 6.0, ((0, 16), (1, 16))),
        "out_gate": gaussian(splits[3], (SEQ, HEADS, HEAD_DIM), 1.0, 6.0, ((0, 16), (1, 16))),
        "decay_rate": draw_decay_rate(jax.random.fold_in(splits[18], 71), 0),
        "decay_pre": draw_decay_pre(jax.random.fold_in(splits[18], 71), 0),
        "decay_shock": draw_decay_shock(jax.random.fold_in(splits[18], 71), 0),
        "beta_pre": draw_beta_pre(jax.random.fold_in(splits[18], 71), 0),
        "head_gain": jnp.clip(1.0 + 0.18 * jax.random.normal(splits[8], (HEAD_DIM,), jnp.float32), 0.1, 1.9),
        "w_out": gaussian(splits[9], (HEADS * HEAD_DIM, D), (HEADS * HEAD_DIM) ** -0.5, 0.125, ((0, 16),)),
        "tokens": gaussian(splits[10], (SEQ, D), 1.0, 6.0, ((0, 256),)),
        "norm_gain": jnp.clip(1.0 + 0.18 * jax.random.normal(splits[11], (D,), jnp.float32), 0.1, 1.9),
        "experts_pick": draw_experts_pick(jax.random.fold_in(splits[18], 71), 0),
        "pair_logits": gaussian(splits[13], (SEQ, 2), 1.5, 6.0, ((0, 256),), jnp.float32),
        "group_logits": gaussian(splits[14], (SEQ, EXPERT_GROUPS), 1.5, 6.0, ((0, 256),), jnp.float32),
        "expert_gate": gaussian(splits[15], (EXPERTS, D, EXP_FF), D ** -0.5, 0.125, ((0, 16), (2, 16))),
        "expert_up": gaussian(splits[16], (EXPERTS, D, EXP_FF), D ** -0.5, 0.125, ((0, 16), (2, 16))),
        "expert_down": gaussian(splits[17], (EXPERTS, D, EXP_FF), (EXP_FF // 16) ** -0.5, 0.5, ((0, 16), (2, 16))),
    }


NORM_EPSILON = 1e-06
EXACT_PRECISION = lax.Precision.HIGHEST

def unit_rows(vectors):
    return vectors * lax.rsqrt(lax.optimization_barrier(jnp.sum(vectors * vectors, axis=-1, keepdims=True)) + NORM_EPSILON)

def block_sweep(queries, key_rows, value_rows, log_decay, beta_rate, start_state):
    length, value_width = value_rows.shape
    blocks = length // BLOCK
    query_blocks = queries.reshape(blocks, BLOCK, queries.shape[1])
    key_blocks = key_rows.reshape(blocks, BLOCK, key_rows.shape[1])
    value_blocks = value_rows.reshape(blocks, BLOCK, value_width)
    cumulative = jnp.cumsum(log_decay.reshape(blocks, BLOCK), axis=1)
    beta_blocks = beta_rate.reshape(blocks, BLOCK)
    position = jnp.arange(BLOCK)
    lower_mask = position[:, None] >= position[None, :]
    strict = position[:, None] > position[None, :]
    spread = cumulative[:, :, None] - cumulative[:, None, :]
    within = jnp.where(lower_mask, jnp.exp(jnp.where(lower_mask, spread, 0.0)), 0.0)
    scaled_keys = key_blocks * beta_blocks[:, :, None]
    lower_matrix = jnp.where(strict, jnp.einsum('nid,njd->nij', scaled_keys, key_blocks, precision=EXACT_PRECISION) * within, 0.0)
    identity = jnp.eye(BLOCK, dtype=jnp.float32)
    right_side = jnp.concatenate([value_blocks * beta_blocks[:, :, None], scaled_keys * jnp.exp(cumulative)[:, :, None]], axis=2)
    solved = jax.scipy.linalg.solve_triangular(lower_matrix + identity, right_side, lower=True, unit_diagonal=True)
    fresh_values = solved[:, :, :value_width]
    corrections = solved[:, :, value_width:]
    scores = jnp.einsum('nid,njd->nij', query_blocks, key_blocks, precision=EXACT_PRECISION) * within
    query_decayed = query_blocks * jnp.exp(cumulative)[:, :, None]
    block_total = cumulative[:, -1]
    decayed_keys = key_blocks * jnp.exp(block_total[:, None] - cumulative)[:, :, None]

    def advance(carried, inputs):
        values_in, fix_rows, query_in, key_in, score_in, total_in = inputs
        updated = values_in - jnp.dot(fix_rows, carried, precision=EXACT_PRECISION)
        output = jnp.dot(query_in, carried, precision=EXACT_PRECISION) + jnp.dot(score_in, updated, precision=EXACT_PRECISION)
        carried = carried * jnp.exp(total_in) + jnp.dot(key_in.T, updated, precision=EXACT_PRECISION)
        return (carried, output)
    final_state, outputs = lax.scan(advance, start_state, (fresh_values, corrections, query_decayed, decayed_keys, scores, block_total))
    return (outputs.reshape(length, value_width), final_state)

def reference(query_vectors, key_vectors, value_vectors, out_gate, decay_rate, decay_pre, decay_shock, beta_pre, head_gain, w_out, tokens, norm_gain, experts_pick, pair_logits, group_logits, expert_gate, expert_up, expert_down):
    queries = unit_rows(jnp.transpose(query_vectors.astype(jnp.float32), (1, 0, 2))) * HEAD_DIM ** (-0.5)
    keyset = unit_rows(jnp.transpose(key_vectors.astype(jnp.float32), (1, 0, 2)))
    valueset = jnp.transpose(value_vectors.astype(jnp.float32), (1, 0, 2))
    log_decay = -decay_rate[:, :, None] * jax.nn.softplus(decay_pre) + decay_shock
    beta_rate = jax.nn.sigmoid(beta_pre)
    zero_state = jnp.zeros((HEAD_DIM, HEAD_DIM), jnp.float32)

    def one_head(packed):
        query_head, key_head, value_head, decay_head, beta_head = packed
        forward_result, _ = block_sweep(query_head, key_head, value_head, decay_head[0], beta_head[0], zero_state)
        trailing_part, _ = block_sweep(query_head[::-1], key_head[::-1], value_head[::-1], decay_head[1, ::-1], beta_head[1, ::-1], zero_state)
        return forward_result + trailing_part[::-1]
    joined = lax.map(one_head, (queries, keyset, valueset, jnp.moveaxis(log_decay, 1, 0), jnp.moveaxis(beta_rate, 1, 0)))
    joined = jnp.transpose(joined, (1, 0, 2))
    head_scale = lax.rsqrt(lax.optimization_barrier(jnp.mean(joined * joined, axis=-1, keepdims=True)) + NORM_EPSILON)
    mixed_heads = (joined * head_scale * head_gain * jax.nn.silu(out_gate.astype(jnp.float32))).astype(jnp.bfloat16)
    mixed_heads = mixed_heads.reshape(SEQ, HEADS * HEAD_DIM)
    group_width = HEADS * HEAD_DIM // N_TP

    def add_heads(running, group_index):
        columns = lax.dynamic_slice_in_dim(mixed_heads, group_index * group_width, group_width, 1)
        weight_rows = lax.dynamic_slice_in_dim(w_out, group_index * group_width, group_width, 0)
        part_sum = jnp.dot(columns.astype(jnp.float32), weight_rows.astype(jnp.float32), preferred_element_type=jnp.float32).astype(jnp.bfloat16)
        return (running + lax.optimization_barrier(part_sum).astype(jnp.float32), None)
    branch_sum, _ = lax.scan(add_heads, jnp.zeros((SEQ, D), jnp.float32), jnp.arange(N_TP, dtype=jnp.int32))
    residual = tokens.astype(jnp.float32) + branch_sum
    normed = (residual * lax.rsqrt(lax.optimization_barrier(jnp.mean(residual * residual, axis=-1, keepdims=True)) + NORM_EPSILON) * norm_gain).astype(jnp.bfloat16)
    group_exp = jnp.exp(group_logits)
    group_share = group_exp / lax.optimization_barrier(jnp.sum(group_exp, axis=-1, keepdims=True))
    group_index_of = experts_pick[:, 0] // GROUP_SIZE
    group_weight = lax.optimization_barrier(jnp.sum(jnp.where(jnp.arange(EXPERT_GROUPS)[None, :] == group_index_of[:, None], group_share, 0.0), axis=1))
    pair_exp = jnp.exp(pair_logits)
    route_weight = pair_exp / lax.optimization_barrier(jnp.sum(pair_exp, axis=-1, keepdims=True)) * group_weight[:, None]
    block_count = SEQ // TOK_DEV
    expert_marks = lax.optimization_barrier(jnp.sum((experts_pick[:, :, None] == jnp.arange(EXPERTS, dtype=jnp.int32)[None, None, :]).astype(jnp.int32), axis=1))
    expert_marks = expert_marks.reshape(block_count, TOK_DEV, EXPERTS)
    earlier = (jnp.cumsum(expert_marks, axis=1) - expert_marks).reshape(SEQ, EXPERTS)
    slot_number = jnp.take_along_axis(earlier, experts_pick, axis=1)
    token_index = jnp.arange(SEQ, dtype=jnp.int32)
    slot_place = (token_index // TOK_DEV)[:, None] * CAP + slot_number
    buffer_rows = block_count * CAP
    slice_width = EXP_FF // N_TP
    sources = jnp.broadcast_to(token_index[:, None], (SEQ, 2)).reshape(-1)

    def add_expert(running, expert):
        expert_hits = experts_pick == expert
        target = jnp.where(expert_hits, slot_place, buffer_rows).reshape(-1).astype(jnp.int32)
        slot_table = jnp.zeros((buffer_rows,), jnp.int32).at[target].set(sources, mode='drop')
        picked = normed[slot_table]
        gate_out = jnp.dot(picked.astype(jnp.float32), expert_gate[expert].astype(jnp.float32), preferred_element_type=jnp.float32)
        up_out = jnp.dot(picked.astype(jnp.float32), expert_up[expert].astype(jnp.float32), preferred_element_type=jnp.float32)
        hidden = (jax.nn.silu(gate_out) * up_out).astype(jnp.bfloat16)
        down_full = expert_down[expert]

        def add_slice(partial_value, slice_index):
            hidden_part = lax.dynamic_slice_in_dim(hidden, slice_index * slice_width, slice_width, 1)
            down_part = lax.dynamic_slice_in_dim(down_full, slice_index * slice_width, slice_width, 1)
            product = lax.dot_general(hidden_part.astype(jnp.float32), down_part.astype(jnp.float32), (((1,), (1,)), ((), ())), preferred_element_type=jnp.float32).astype(jnp.bfloat16)
            return (partial_value + lax.optimization_barrier(product).astype(jnp.float32), None)
        summed_out, _ = lax.scan(add_slice, jnp.zeros((buffer_rows, D), jnp.float32), jnp.arange(N_TP, dtype=jnp.int32))
        answer = summed_out.astype(jnp.bfloat16)
        first_hit = expert_hits[:, 0]
        row_of = jnp.where(first_hit, slot_place[:, 0], slot_place[:, 1]).astype(jnp.int32)
        weight_of = jnp.where(first_hit, route_weight[:, 0], jnp.where(expert_hits[:, 1], route_weight[:, 1], 0.0))
        return (running + weight_of[:, None] * answer[row_of].astype(jnp.float32), None)
    mixture, _ = lax.scan(add_expert, jnp.zeros((SEQ, D), jnp.float32), jnp.arange(EXPERTS, dtype=jnp.int32))
    return (residual + mixture).astype(jnp.bfloat16)
```

```python
import jax
import jax.numpy as jnp
from jax import lax
from jax.experimental import pallas as pl
from jax.experimental.pallas import tpu as pltpu
from jax.sharding import Mesh
from jax.sharding import PartitionSpec as P

CHUNK = 128
GROUP_SIZE = 2
EPS = 1e-06
SP = ("sp_0", "sp_1")
SP_TP = ("sp_0", "sp_1", "tp")
F32 = jnp.float32
BF16 = jnp.bfloat16
PAIRED = 2


def mm(a, b):
    return jnp.dot(a, b, preferred_element_type=F32)


def mm_nt(a, b):
    return lax.dot_general(a, b, (((1,), (1,)), ((), ())), preferred_element_type=F32)


def iota2(shape, dim):
    return lax.broadcasted_iota(jnp.int32, shape, dim)


def local_kernel(rate_ref, q_ref, k_ref, v_ref, pre_ref, shock_ref, bpre_ref,
                 out_ref, reach_ref, maps_ref,
                 mask_ref, row_ref, col_ref, qeff_ref, add_ref, cut_ref):
    C = CHUNK
    length = q_ref.shape[0]
    chunks = length // C
    dh = q_ref.shape[1]
    scale = dh ** -0.5
    row = iota2((C, C), 0)
    col = iota2((C, C), 1)
    spans = []
    span = 1
    while span < C:
        spans.append(span)
        span *= 2
    for level, span in enumerate(spans):
        same = (row // (2 * span)) == (col // (2 * span))
        lower = same & ((row // span) % 2 == 1) & ((col // span) % 2 == 0)
        upper = same & ((row // span) % 2 == 0) & ((col // span) % 2 == 1)
        mask_ref[0, level] = lower.astype(F32).astype(BF16)
        mask_ref[1, level] = upper.astype(F32).astype(BF16)

    rows = 2 * chunks
    first = iota2((rows, C), 0) < chunks
    rate = jnp.where(first, rate_ref[0, 0], rate_ref[1, 0])
    pre = pre_ref[...]
    soft = jnp.maximum(pre, 0.0) + jnp.log1p(jnp.exp(-jnp.abs(pre)))
    decay = -rate * soft + shock_ref[...]
    beta = 1.0 / (1.0 + jnp.exp(-bpre_ref[...]))
    tri = (row <= col).astype(F32)
    tri_back = (row >= col).astype(F32)
    ahead = jnp.dot(decay, tri, precision=lax.Precision.HIGHEST, preferred_element_type=F32)
    behind = jnp.dot(decay, tri_back, precision=lax.Precision.HIGHEST, preferred_element_type=F32)
    summed = jnp.where(first, ahead, behind)
    total = jnp.where(first[:, :1], summed[:, C - 1:], summed[:, :1])
    row_ref[0] = summed
    row_ref[1] = beta
    row_ref[2] = beta * jnp.exp(summed)
    row_ref[3] = jnp.broadcast_to(jnp.exp(total), (rows, C))
    stacked = jnp.concatenate([summed, beta, jnp.exp(summed), jnp.exp(total - summed)], axis=0)
    stacked = jnp.concatenate([stacked, jnp.zeros((C - 4 * rows, C), F32)], axis=0) if 4 * rows < C else stacked
    turned = stacked.T
    for part in range(4):
        for r in range(rows):
            if part == 0:
                col_ref[part, r] = jnp.broadcast_to(turned[:, r:r + 1], (C, C))
            else:
                col_ref[part, r] = jnp.broadcast_to(turned[:, part * rows + r:part * rows + r + 1], (C, C))

    eye = (row == col).astype(F32)

    def body(step, carry):
        work = []
        for u in range(PAIRED):
            n = step * PAIRED + u
            here = pl.ds(pl.multiple_of(n * C, C), C)
            q = q_ref[here, :].astype(F32)
            k = k_ref[here, :].astype(F32)
            v = v_ref[here, :]
            qn = q * lax.rsqrt(jnp.sum(q * q, axis=1, keepdims=True) + EPS) * scale
            kn = k * lax.rsqrt(jnp.sum(k * k, axis=1, keepdims=True) + EPS)
            kb = kn.astype(BF16)
            qb = qn.astype(BF16)
            gram = mm_nt(kb, kb)
            score = mm_nt(qb, kb)
            kt = kn.T.astype(BF16)
            for d in range(2):
                r = d * chunks + n
                work.append(dict(d=d, r=r, n=n, qn=qn, kb=kb, v=v, kt=kt, gram=gram, score=score))
        for w in work:
            d, r = w["d"], w["r"]
            keep = (row >= col) if d == 0 else (row <= col)
            strict = (row > col) if d == 0 else (row < col)
            diff = col_ref[0, r] - row_ref[0, pl.ds(r, 1), :]
            within = jnp.where(keep, jnp.exp(jnp.where(keep, diff, 0.0)), 0.0)
            a = jnp.where(strict, w["gram"] * within * col_ref[1, r], 0.0).astype(BF16)
            w["a"] = a
            w["p"] = (w["score"] * within).astype(BF16)
            w["t"] = eye - (a * mask_ref[d, 0]).astype(F32)
        for level in range(1, len(spans)):
            for w in work:
                w["tb"] = w["t"].astype(BF16)
                w["x"] = mm(w["a"] * mask_ref[w["d"], level], w["tb"]).astype(BF16)
            for w in work:
                w["t"] = w["t"] - mm(w["tb"], w["x"])
        for w in work:
            r = w["r"]
            fresh = mm((w["t"] * row_ref[1, pl.ds(r, 1), :]).astype(BF16), w["v"])
            fix = mm((w["t"] * row_ref[2, pl.ds(r, 1), :]).astype(BF16), w["kb"])
            w["uw"] = jnp.concatenate([fresh, fix], axis=1)
        for w in work:
            r, d, n = w["r"], w["d"], w["n"]
            pu = mm(w["p"], w["uw"].astype(BF16))
            w["local"] = pu[:, :dh]
            qeff_ref[r] = (w["qn"] * col_ref[2, r] - pu[:, dh:]).astype(BF16)
            faded = col_ref[3, r]
            bk = mm(w["kt"], (w["uw"] * jnp.concatenate([faded, faded], axis=1)).astype(BF16))
            add_ref[r] = bk[:, :dh]
            cut_ref[r] = bk[:, dh:].astype(BF16)
        for u in range(PAIRED):
            n = step * PAIRED + u
            here = pl.ds(pl.multiple_of(n * C, C), C)
            out_ref[here, :] = work[2 * u]["local"] + work[2 * u + 1]["local"]
        return carry

    lax.fori_loop(0, chunks // PAIRED, body, 0)

    z = [jnp.concatenate([jnp.zeros((dh, dh), F32), eye], axis=1) for _ in range(2)]
    for step in range(chunks):
        for d in range(2):
            n = step if d == 0 else chunks - 1 - step
            r = d * chunks + n
            zb = z[d].astype(BF16)
            seen = mm(qeff_ref[r], zb)
            out_ref[n * C:(n + 1) * C, :] += seen[:, :dh]
            reach_ref[n * C:(n + 1) * C, d * dh:(d + 1) * dh] = seen[:, dh:].astype(BF16)
            keep = row_ref[3, r:r + 1, :]
            moved = mm(cut_ref[r], zb)
            z[d] = jnp.concatenate([z[d][:, :dh] * keep - moved[:, :dh] + add_ref[r],
                                    z[d][:, dh:] * keep - moved[:, dh:]], axis=1)
    for d in range(2):
        maps_ref[d] = z[d].astype(BF16)


def local_attention(q, k, v, rate, pre, shock, bpre):
    length, dh = q.shape
    chunks = length // CHUNK
    levels = CHUNK.bit_length() - 1
    vm = pl.BlockSpec(memory_space=pltpu.VMEM)
    return pl.pallas_call(
        local_kernel,
        out_shape=(
            jax.ShapeDtypeStruct((length, dh), F32),
            jax.ShapeDtypeStruct((length, 2 * dh), BF16),
            jax.ShapeDtypeStruct((2, dh, 2 * dh), BF16),
        ),
        in_specs=[pl.BlockSpec(memory_space=pltpu.SMEM)] + [vm] * 6,
        out_specs=(vm, vm, vm),
        scratch_shapes=[
            pltpu.VMEM((2, levels, CHUNK, CHUNK), BF16),
            pltpu.VMEM((4, 2 * chunks, CHUNK), F32),
            pltpu.VMEM((4, 2 * chunks, CHUNK, CHUNK), F32),
            pltpu.VMEM((2 * chunks, CHUNK, dh), BF16),
            pltpu.VMEM((2 * chunks, dh, dh), F32),
            pltpu.VMEM((2 * chunks, dh, dh), BF16),
        ],
        name="local_attention",
    )(rate, q, k, v, pre, shock, bpre)


def compose_kernel(where_ref, own_ref, one_ref, two_ref, three_ref, before_ref, all_ref, line_ref):
    dh = own_ref.shape[1]
    here = where_ref[0]
    for distance, ref in enumerate((own_ref, one_ref, two_ref, three_ref)):
        line_ref[lax.rem(here + 4 - distance, 4)] = ref[...]
    zero = jnp.concatenate(
        [jnp.zeros((dh, dh), F32), (iota2((dh, dh), 0) == iota2((dh, dh), 1)).astype(F32)], axis=1
    )
    for d in range(2):
        z = zero
        before = zero
        order = range(4) if d == 0 else range(3, -1, -1)
        for step, j in enumerate(order):
            before = jnp.where(here == j, z, before)
            added = line_ref[j, d, :, :dh].astype(F32)
            if step == 0:
                z = line_ref[j, d].astype(F32)
            else:
                moved = mm(line_ref[j, d, :, dh:], z.astype(BF16))
                z = jnp.concatenate([moved[:, :dh] + added, moved[:, dh:]], axis=1)
        before_ref[d] = before.astype(BF16)
        all_ref[d] = z.astype(BF16)


def compose_line(where, own, others):
    vm = pl.BlockSpec(memory_space=pltpu.VMEM)
    return pl.pallas_call(
        compose_kernel,
        out_shape=(jax.ShapeDtypeStruct(own.shape, BF16), jax.ShapeDtypeStruct(own.shape, BF16)),
        in_specs=[pl.BlockSpec(memory_space=pltpu.SMEM)] + [vm] * 4,
        out_specs=(vm, vm),
        scratch_shapes=[pltpu.VMEM((4,) + own.shape, BF16)],
        name="compose_line",
    )(where, own, *others)


def mix_kernel(where_ref, before_ref, own_ref, one_ref, two_ref, three_ref, local_ref, reach_ref,
               gate_ref, gain_ref, mixed_ref, line_ref, state_ref):
    dh = local_ref.shape[1]
    here = where_ref[0]
    for distance, ref in enumerate((own_ref, one_ref, two_ref, three_ref)):
        line_ref[lax.rem(here + 4 - distance, 4)] = ref[...]
    for d in range(2):
        s = jnp.zeros((dh, dh), F32)
        order = (0, 1, 2) if d == 0 else (3, 2, 1)
        for step, j in enumerate(order):
            passed = (j < here) if d == 0 else (j > here)
            added = line_ref[j, d, :, :dh].astype(F32)
            if step == 0:
                new = added
            else:
                new = mm(line_ref[j, d, :, dh:], s.astype(BF16)) + added
            s = jnp.where(passed, new, s)
        s = mm(before_ref[d, :, dh:], s.astype(BF16)) + before_ref[d, :, :dh].astype(F32)
        state_ref[d * dh:(d + 1) * dh, :] = s.astype(BF16)
    gain = gain_ref[...]
    block = 256
    for i in range(local_ref.shape[0] // block):
        here_rows = slice(i * block, (i + 1) * block)
        joined = local_ref[here_rows, :] + mm(reach_ref[here_rows, :], state_ref[...])
        gate = gate_ref[here_rows, :].astype(F32)
        gate = gate / (1.0 + jnp.exp(-gate))
        mean = jnp.mean(joined * joined, axis=1, keepdims=True)
        mixed_ref[here_rows, :] = (joined * lax.rsqrt(mean + EPS) * gain * gate).astype(BF16)


def mix_heads(where, before, own, others, local, reach, gate, gain):
    vm = pl.BlockSpec(memory_space=pltpu.VMEM)
    dh = local.shape[1]
    return pl.pallas_call(
        mix_kernel,
        out_shape=jax.ShapeDtypeStruct(local.shape, BF16),
        in_specs=[pl.BlockSpec(memory_space=pltpu.SMEM)] + [vm] * 9,
        out_specs=vm,
        scratch_shapes=[pltpu.VMEM((4,) + own.shape, BF16), pltpu.VMEM((2 * dh, dh), BF16)],
        name="mix_heads",
    )(where, before, own, *others, local, reach, gate, gain)


def project_kernel(own_ref, one_ref, two_ref, three_ref, w_ref, o0, o1, o2, o3):
    rows = own_ref.shape[0]
    stacked = jnp.concatenate([own_ref[...], one_ref[...], two_ref[...], three_ref[...]], axis=0)
    parts = mm(stacked, w_ref[...]).astype(BF16)
    for i, ref in enumerate((o0, o1, o2, o3)):
        ref[...] = parts[i * rows:(i + 1) * rows]


def project(blocks, weight):
    vm = pl.BlockSpec(memory_space=pltpu.VMEM)
    shape = jax.ShapeDtypeStruct((blocks[0].shape[0], weight.shape[1]), BF16)
    return pl.pallas_call(
        project_kernel, out_shape=(shape,) * 4, in_specs=[vm] * 5, out_specs=(vm,) * 4,
        name="project",
    )(*blocks, weight)


def route_kernel(where_ref, p0, p1, p2, p3, tokens_ref, gain_ref, slots_ref, residual_ref, outgoing_ref, line_ref):
    here = where_ref[0]
    for distance, ref in enumerate((p0, p1, p2, p3)):
        line_ref[lax.rem(here + distance, 4)] = ref[...]
    branch = jnp.concatenate([line_ref[j] for j in range(4)], axis=1).astype(F32)
    residual = tokens_ref[...].astype(F32) + branch
    residual_ref[...] = residual
    mean = jnp.mean(residual * residual, axis=1, keepdims=True)
    normed = (residual * lax.rsqrt(mean + EPS) * gain_ref[...]).astype(BF16)
    count = outgoing_ref.shape[0]
    slot = iota2((count, residual.shape[0]), 0)
    chooser = ((slot == slots_ref[0:1, :]) | (slot == slots_ref[1:2, :])).astype(F32).astype(BF16)
    outgoing_ref[...] = mm(chooser, normed).astype(BF16)


def route(where, parts, tokens, gain, slots, count):
    vm = pl.BlockSpec(memory_space=pltpu.VMEM)
    return pl.pallas_call(
        route_kernel,
        out_shape=(
            jax.ShapeDtypeStruct(tokens.shape, F32),
            jax.ShapeDtypeStruct((count, tokens.shape[1]), BF16),
        ),
        in_specs=[pl.BlockSpec(memory_space=pltpu.SMEM)] + [vm] * 7,
        out_specs=(vm, vm),
        scratch_shapes=[pltpu.VMEM((4,) + parts[0].shape, BF16)],
        name="route",
    )(where, *parts, tokens, gain, slots)


def expert_kernel(rows_ref, w_ref, out_ref, sum_ref):
    j = pl.program_id(0)

    @pl.when(j == 0)
    def _():
        sum_ref[...] = jnp.zeros_like(sum_ref)

    width = w_ref.shape[3]
    both = mm(rows_ref[...], jnp.concatenate([w_ref[0, 0], w_ref[0, 1]], axis=1))
    gate = both[:, :width]
    hidden = (gate / (1.0 + jnp.exp(-gate)) * both[:, width:]).astype(BF16)
    sum_ref[...] += mm_nt(hidden, w_ref[0, 2])

    @pl.when(j == pl.num_programs(0) - 1)
    def _():
        out_ref[...] = sum_ref[...].astype(BF16)


def run_expert(rows, weights):
    count, _, width, part = weights.shape
    return pl.pallas_call(
        expert_kernel,
        out_shape=jax.ShapeDtypeStruct(rows.shape, BF16),
        grid=(count,),
        in_specs=[
            pl.BlockSpec(rows.shape, lambda j: (0, 0)),
            pl.BlockSpec((1, 3, width, part), lambda j: (j, 0, 0, 0)),
        ],
        out_specs=pl.BlockSpec(rows.shape, lambda j: (0, 0)),
        scratch_shapes=[pltpu.VMEM(rows.shape, F32)],
        compiler_params=pltpu.CompilerParams(dimension_semantics=("arbitrary",)),
        name="run_expert",
    )(rows, weights)


def finish_kernel(residual_ref, rows_ref, slots_ref, weight_ref, out_ref):
    tokens = residual_ref.shape[0]
    count = rows_ref.shape[0]
    slot = iota2((tokens, count), 1)
    chosen = jnp.where(slot == slots_ref[:, 0:1], weight_ref[:, 0:1], 0.0) + jnp.where(
        slot == slots_ref[:, 1:2], weight_ref[:, 1:2], 0.0
    )
    high = chosen.astype(BF16)
    low = (chosen - high.astype(F32)).astype(BF16)
    rows = rows_ref[...]
    out_ref[...] = (residual_ref[...] + (mm(high, rows) + mm(low, rows))).astype(BF16)


def finish(residual, rows, slots, weight):
    vm = pl.BlockSpec(memory_space=pltpu.VMEM)
    return pl.pallas_call(
        finish_kernel,
        out_shape=jax.ShapeDtypeStruct(residual.shape, BF16),
        in_specs=[vm] * 4,
        out_specs=vm,
        name="finish",
    )(residual, rows, slots, weight)


def around(x, axis):
    size = lax.axis_size(axis)
    return [lax.ppermute(x, axis, [(i, (i + d) % size) for i in range(size)]) for d in range(1, size)]


def shards(
    query_vectors, key_vectors, value_vectors, out_gate, decay_rate, decay_pre, decay_shock, beta_pre,
    head_gain, w_out, tokens, norm_gain, experts_pick, pair_logits, group_logits,
    expert_gate, expert_up, expert_down,
):
    length, _, dh = query_vectors.shape
    chunks = length // CHUNK
    at_x = lax.axis_index("sp_1")
    at_y = lax.axis_index("sp_0")
    where_x = at_x.astype(jnp.int32).reshape(1)
    where_y = at_y.astype(jnp.int32).reshape(1)

    quarter = w_out.shape[1] // lax.axis_size("sp_1")
    w_part = lax.dynamic_slice_in_dim(w_out, at_x * quarter, quarter, 1)
    w_columns = lax.all_gather(w_part, "tp", axis=0, tiled=True)
    experts = jnp.concatenate([expert_gate, expert_up, expert_down], axis=0)
    experts, w_columns = lax.optimization_barrier((experts, w_columns)) if False else (experts, w_columns)
    expert_all = lax.all_gather(experts, "tp", axis=0)

    local_rows = tokens.shape[0]
    group_count = group_logits.shape[1]
    group_exp = jnp.exp(group_logits)
    group_share = group_exp / jnp.sum(group_exp, axis=-1, keepdims=True)
    group_index_of = experts_pick[:, 0] // GROUP_SIZE
    group_weight = jnp.sum(
        jnp.where(jnp.arange(group_count)[None, :] == group_index_of[:, None], group_share, 0.0), axis=1
    )
    pair_exp = jnp.exp(pair_logits)
    route_weight = pair_exp / jnp.sum(pair_exp, axis=-1, keepdims=True) * group_weight[:, None]
    capacity = local_rows // group_count
    expert_count = lax.axis_size(SP)
    expert_marks = jnp.sum(
        (experts_pick[:, :, None] == jnp.arange(expert_count, dtype=jnp.int32)[None, None, :]).astype(jnp.int32),
        axis=1,
    )
    before_me = (jnp.arange(local_rows)[None, :] < jnp.arange(local_rows)[:, None]).astype(BF16)
    earlier = jnp.dot(before_me, expert_marks.astype(BF16), preferred_element_type=F32).astype(jnp.int32)
    slot_in = jnp.sum(
        jnp.where(
            experts_pick[:, :, None] == jnp.arange(expert_count, dtype=jnp.int32)[None, None, :],
            earlier[:, None, :], 0,
        ),
        axis=2,
    )
    slot_place = experts_pick * capacity + slot_in

    local, reach, maps = local_attention(
        query_vectors.reshape(length, dh), key_vectors.reshape(length, dh), value_vectors.reshape(length, dh),
        decay_rate,
        decay_pre.reshape(2 * chunks, CHUNK), decay_shock.reshape(2 * chunks, CHUNK),
        beta_pre.reshape(2 * chunks, CHUNK),
    )
    before, line = compose_line(where_x, maps, around(maps, "sp_1"))
    mixed = mix_heads(
        where_y, before, line, around(line, "sp_0"), local, reach,
        out_gate.reshape(length, dh), head_gain.reshape(1, dh),
    )
    mine = lax.all_to_all(mixed, "tp", split_axis=0, concat_axis=1, tiled=True)
    parts = project([mine] + around(mine, "sp_1"), w_columns)
    size = lax.axis_size("sp_1")
    returned = [parts[0]] + [
        lax.ppermute(parts[d], "sp_1", [(i, (i - d) % size) for i in range(size)]) for d in range(1, size)
    ]
    residual, outgoing = route(
        where_x, returned, tokens, norm_gain.reshape(1, -1), slot_place.T, expert_count * capacity
    )
    width = outgoing.shape[1]
    outgoing = outgoing.reshape(expert_count, capacity, width)
    arrived = lax.all_to_all(outgoing, SP, split_axis=0, concat_axis=0, tiled=True)
    expert_rows = run_expert(arrived.reshape(expert_count * capacity, width), expert_all)
    expert_rows = expert_rows.reshape(expert_count, capacity, width)
    results = lax.all_to_all(expert_rows, SP, split_axis=0, concat_axis=0, tiled=True)
    return finish(residual, results.reshape(expert_count * capacity, width), slot_place, route_weight)


def solution(mesh):
    finer = Mesh(mesh.devices.reshape(4, 4, mesh.shape["tp"]), ("sp_0", "sp_1", "tp"))
    in_specs = (
        P(SP, "tp", None), P(SP, "tp", None), P(SP, "tp", None), P(SP, "tp", None),
        P(None, "tp"),
        P(None, "tp", SP), P(None, "tp", SP), P(None, "tp", SP),
        P(), P("tp", None), P(SP_TP, None), P(),
        P(SP_TP, None), P(SP_TP, None), P(SP_TP, None),
        P(SP, None, "tp"), P(SP, None, "tp"), P(SP, None, "tp"),
    )
    return jax.shard_map(
        shards, mesh=finer, in_specs=in_specs, out_specs=P(SP_TP, None), check_vma=False
    )
```

```python
import jax
import jax.numpy as jnp
from jax import lax
from jax.experimental import pallas as pl
from jax.experimental.pallas import tpu as pltpu
from jax.sharding import Mesh
from jax.sharding import PartitionSpec as P

CHUNK = 128
GROUP_SIZE = 2
EPS = 1e-06
SP = ("sp_0", "sp_1")
SP_TP = ("sp_0", "sp_1", "tp")
F32 = jnp.float32
BF16 = jnp.bfloat16
PAIRED = 2


def mm(a, b):
    return jnp.dot(a, b, preferred_element_type=F32)


def mm_nt(a, b):
    return lax.dot_general(a, b, (((1,), (1,)), ((), ())), preferred_element_type=F32)


def iota2(shape, dim):
    return lax.broadcasted_iota(jnp.int32, shape, dim)


def local_kernel(rate_ref, q_ref, k_ref, v_ref, pre_ref, shock_ref, bpre_ref,
                 out_ref, reach_ref, maps_ref,
                 mask_ref, row_ref, col_ref, qeff_ref, add_ref, cut_ref):
    C = CHUNK
    length = q_ref.shape[0]
    chunks = length // C
    dh = q_ref.shape[1]
    scale = dh ** -0.5
    row = iota2((C, C), 0)
    col = iota2((C, C), 1)
    spans = []
    span = 1
    while span < C:
        spans.append(span)
        span *= 2
    for level, span in enumerate(spans):
        same = (row // (2 * span)) == (col // (2 * span))
        lower = same & ((row // span) % 2 == 1) & ((col // span) % 2 == 0)
        upper = same & ((row // span) % 2 == 0) & ((col // span) % 2 == 1)
        mask_ref[0, level] = lower.astype(F32).astype(BF16)
        mask_ref[1, level] = upper.astype(F32).astype(BF16)

    rows = 2 * chunks
    first = iota2((rows, C), 0) < chunks
    rate = jnp.where(first, rate_ref[0, 0], rate_ref[1, 0])
    pre = pre_ref[...]
    soft = jnp.maximum(pre, 0.0) + jnp.log1p(jnp.exp(-jnp.abs(pre)))
    decay = -rate * soft + shock_ref[...]
    beta = 1.0 / (1.0 + jnp.exp(-bpre_ref[...]))
    tri = (row <= col).astype(F32)
    tri_back = (row >= col).astype(F32)
    ahead = jnp.dot(decay, tri, precision=lax.Precision.HIGHEST, preferred_element_type=F32)
    behind = jnp.dot(decay, tri_back, precision=lax.Precision.HIGHEST, preferred_element_type=F32)
    summed = jnp.where(first, ahead, behind)
    total = jnp.where(first[:, :1], summed[:, C - 1:], summed[:, :1])
    row_ref[0] = summed
    row_ref[1] = beta
    row_ref[2] = beta * jnp.exp(summed)
    row_ref[3] = jnp.broadcast_to(jnp.exp(total), (rows, C))
    stacked = jnp.concatenate([summed, beta, jnp.exp(summed), jnp.exp(total - summed)], axis=0)
    stacked = jnp.concatenate([stacked, jnp.zeros((C - 4 * rows, C), F32)], axis=0) if 4 * rows < C else stacked
    turned = stacked.T
    for part in range(4):
        for r in range(rows):
            if part == 0:
                col_ref[part, r] = jnp.broadcast_to(turned[:, r:r + 1], (C, C))
            else:
                col_ref[part, r] = jnp.broadcast_to(turned[:, part * rows + r:part * rows + r + 1], (C, C))

    eye = (row == col).astype(F32)

    def body(step, carry):
        work = []
        for u in range(PAIRED):
            n = step * PAIRED + u
            here = pl.ds(pl.multiple_of(n * C, C), C)
            q = q_ref[here, :].astype(F32)
            k = k_ref[here, :].astype(F32)
            v = v_ref[here, :]
            qn = q * lax.rsqrt(jnp.sum(q * q, axis=1, keepdims=True) + EPS) * scale
            kn = k * lax.rsqrt(jnp.sum(k * k, axis=1, keepdims=True) + EPS)
            kb = kn.astype(BF16)
            qb = qn.astype(BF16)
            gram = mm_nt(kb, kb)
            score = mm_nt(qb, kb)
            kt = kn.T.astype(BF16)
            for d in range(2):
                r = d * chunks + n
                work.append(dict(d=d, r=r, n=n, qn=qn, kb=kb, v=v, kt=kt, gram=gram, score=score))
        for w in work:
            d, r = w["d"], w["r"]
            keep = (row >= col) if d == 0 else (row <= col)
            strict = (row > col) if d == 0 else (row < col)
            diff = col_ref[0, r] - row_ref[0, pl.ds(r, 1), :]
            within = jnp.where(keep, jnp.exp(jnp.where(keep, diff, 0.0)), 0.0)
            a = jnp.where(strict, w["gram"] * within * col_ref[1, r], 0.0).astype(BF16)
            w["a"] = a
            w["p"] = (w["score"] * within).astype(BF16)
            w["t"] = eye - (a * mask_ref[d, 0]).astype(F32)
        for level in range(1, len(spans)):
            for w in work:
                w["tb"] = w["t"].astype(BF16)
                w["x"] = mm(w["a"] * mask_ref[w["d"], level], w["tb"]).astype(BF16)
            for w in work:
                w["t"] = w["t"] - mm(w["tb"], w["x"])
        for w in work:
            r = w["r"]
            fresh = mm((w["t"] * row_ref[1, pl.ds(r, 1), :]).astype(BF16), w["v"])
            fix = mm((w["t"] * row_ref[2, pl.ds(r, 1), :]).astype(BF16), w["kb"])
            w["uw"] = jnp.concatenate([fresh, fix], axis=1)
        for w in work:
            r, d, n = w["r"], w["d"], w["n"]
            pu = mm(w["p"], w["uw"].astype(BF16))
            w["local"] = pu[:, :dh]
            qeff_ref[r] = (w["qn"] * col_ref[2, r] - pu[:, dh:]).astype(BF16)
            faded = col_ref[3, r]
            bk = mm(w["kt"], (w["uw"] * jnp.concatenate([faded, faded], axis=1)).astype(BF16))
            add_ref[r] = bk[:, :dh]
            cut_ref[r] = bk[:, dh:].astype(BF16)
        for u in range(PAIRED):
            n = step * PAIRED + u
            here = pl.ds(pl.multiple_of(n * C, C), C)
            out_ref[here, :] = work[2 * u]["local"] + work[2 * u + 1]["local"]
        return carry

    lax.fori_loop(0, chunks // PAIRED, body, 0)

    z = [jnp.concatenate([jnp.zeros((dh, dh), F32), eye], axis=1) for _ in range(2)]
    for step in range(chunks):
        for d in range(2):
            n = step if d == 0 else chunks - 1 - step
            r = d * chunks + n
            zb = z[d].astype(BF16)
            seen = mm(qeff_ref[r], zb)
            out_ref[n * C:(n + 1) * C, :] += seen[:, :dh]
            reach_ref[n * C:(n + 1) * C, d * dh:(d + 1) * dh] = seen[:, dh:].astype(BF16)
            keep = row_ref[3, r:r + 1, :]
            moved = mm(cut_ref[r], zb)
            z[d] = jnp.concatenate([z[d][:, :dh] * keep - moved[:, :dh] + add_ref[r],
                                    z[d][:, dh:] * keep - moved[:, dh:]], axis=1)
    for d in range(2):
        maps_ref[d] = z[d].astype(BF16)


def local_attention(q, k, v, rate, pre, shock, bpre):
    length, dh = q.shape
    chunks = length // CHUNK
    levels = CHUNK.bit_length() - 1
    vm = pl.BlockSpec(memory_space=pltpu.VMEM)
    return pl.pallas_call(
        local_kernel,
        out_shape=(
            jax.ShapeDtypeStruct((length, dh), F32),
            jax.ShapeDtypeStruct((length, 2 * dh), BF16),
            jax.ShapeDtypeStruct((2, dh, 2 * dh), BF16),
        ),
        in_specs=[pl.BlockSpec(memory_space=pltpu.SMEM)] + [vm] * 6,
        out_specs=(vm, vm, vm),
        scratch_shapes=[
            pltpu.VMEM((2, levels, CHUNK, CHUNK), BF16),
            pltpu.VMEM((4, 2 * chunks, CHUNK), F32),
            pltpu.VMEM((4, 2 * chunks, CHUNK, CHUNK), F32),
            pltpu.VMEM((2 * chunks, CHUNK, dh), BF16),
            pltpu.VMEM((2 * chunks, dh, dh), F32),
            pltpu.VMEM((2 * chunks, dh, dh), BF16),
        ],
        name="local_attention",
    )(rate, q, k, v, pre, shock, bpre)


def compose_kernel(where_ref, own_ref, one_ref, two_ref, three_ref, before_ref, s1, s2, s3, line_ref):
    dh = own_ref.shape[1]
    here = where_ref[0]
    across = where_ref[1]
    for distance, ref in enumerate((own_ref, one_ref, two_ref, three_ref)):
        line_ref[lax.rem(here + 4 - distance, 4)] = ref[...]
    zero = jnp.concatenate(
        [jnp.zeros((dh, dh), F32), (iota2((dh, dh), 0) == iota2((dh, dh), 1)).astype(F32)], axis=1
    )
    ends = []
    for d in range(2):
        z = zero
        before = zero
        order = range(4) if d == 0 else range(3, -1, -1)
        for step, j in enumerate(order):
            before = jnp.where(here == j, z, before)
            added = line_ref[j, d, :, :dh].astype(F32)
            if step == 0:
                z = line_ref[j, d].astype(F32)
            else:
                moved = mm(line_ref[j, d, :, dh:], z.astype(BF16))
                z = jnp.concatenate([moved[:, :dh] + added, moved[:, dh:]], axis=1)
        before_ref[d] = before.astype(BF16)
        ends.append(z)
    for distance, ref in enumerate((s1, s2, s3), 1):
        ref[...] = jnp.where(across + distance < 4, ends[0], ends[1]).astype(BF16)


def compose_line(where, own, others):
    vm = pl.BlockSpec(memory_space=pltpu.VMEM)
    return pl.pallas_call(
        compose_kernel,
        out_shape=(jax.ShapeDtypeStruct(own.shape, BF16),) + (jax.ShapeDtypeStruct(own.shape[1:], BF16),) * 3,
        in_specs=[pl.BlockSpec(memory_space=pltpu.SMEM)] + [vm] * 4,
        out_specs=(vm,) * 4,
        scratch_shapes=[pltpu.VMEM((4,) + own.shape, BF16)],
        name="compose_line",
    )(where, own, *others)


def mix_kernel(where_ref, before_ref, one_ref, two_ref, three_ref, local_ref, reach_ref,
               gate_ref, gain_ref, mixed_ref, line_ref, state_ref):
    dh = local_ref.shape[1]
    here = where_ref[1]
    for distance, ref in enumerate((one_ref, two_ref, three_ref), 1):
        line_ref[distance] = ref[...]
    line_ref[0] = jnp.zeros_like(one_ref)
    for d in range(2):
        s = jnp.zeros((dh, dh), F32)
        order = (0, 1, 2) if d == 0 else (3, 2, 1)
        for step, j in enumerate(order):
            passed = (j < here) if d == 0 else (j > here)
            piece = lax.rem(here - j + 4, 4)
            new = line_ref[piece, :, :dh].astype(F32)
            if step > 0:
                new = new + mm(line_ref[piece, :, dh:], s.astype(BF16))
            s = jnp.where(passed, new, s)
        s = mm(before_ref[d, :, dh:], s.astype(BF16)) + before_ref[d, :, :dh].astype(F32)
        state_ref[d * dh:(d + 1) * dh, :] = s.astype(BF16)
    gain = gain_ref[...]
    block = 256
    for i in range(local_ref.shape[0] // block):
        here_rows = slice(i * block, (i + 1) * block)
        joined = local_ref[here_rows, :] + mm(reach_ref[here_rows, :], state_ref[...])
        gate = gate_ref[here_rows, :].astype(F32)
        gate = gate / (1.0 + jnp.exp(-gate))
        mean = jnp.mean(joined * joined, axis=1, keepdims=True)
        mixed_ref[here_rows, :] = (joined * lax.rsqrt(mean + EPS) * gain * gate).astype(BF16)


def mix_heads(where, before, others, local, reach, gate, gain):
    vm = pl.BlockSpec(memory_space=pltpu.VMEM)
    dh = local.shape[1]
    return pl.pallas_call(
        mix_kernel,
        out_shape=jax.ShapeDtypeStruct(local.shape, BF16),
        in_specs=[pl.BlockSpec(memory_space=pltpu.SMEM)] + [vm] * 8,
        out_specs=vm,
        scratch_shapes=[pltpu.VMEM((4,) + others[0].shape, BF16), pltpu.VMEM((2 * dh, dh), BF16)],
        name="mix_heads",
    )(where, before, *others, local, reach, gate, gain)


def project_kernel(where_ref, own_ref, one_ref, two_ref, three_ref, w0, w1, w2, w3, o0, o1, o2, o3, line_ref):
    rows = own_ref.shape[0]
    here = where_ref[1]
    stacked = jnp.concatenate([own_ref[...], one_ref[...], two_ref[...], three_ref[...]], axis=0)
    for distance, ref in enumerate((w0, w1, w2, w3)):
        line_ref[lax.rem(here + 4 - distance, 4)] = mm(stacked, ref[...]).astype(BF16)
    for i, ref in enumerate((o0, o1, o2, o3)):
        ref[...] = jnp.concatenate([line_ref[j, i * rows:(i + 1) * rows, :] for j in range(4)], axis=1)


def project(where, blocks, weights):
    vm = pl.BlockSpec(memory_space=pltpu.VMEM)
    rows = blocks[0].shape[0]
    part = weights[0].shape[1]
    shape = jax.ShapeDtypeStruct((rows, 4 * part), BF16)
    return pl.pallas_call(
        project_kernel, out_shape=(shape,) * 4,
        in_specs=[pl.BlockSpec(memory_space=pltpu.SMEM)] + [vm] * 8, out_specs=(vm,) * 4,
        scratch_shapes=[pltpu.VMEM((4, 4 * rows, part), BF16)],
        name="project",
    )(where, *blocks, *weights)


def route_kernel(where_ref, p0, p1, p2, p3, tokens_ref, gain_ref, slots_ref, residual_ref, outgoing_ref, line_ref):
    here = where_ref[0]
    for distance, ref in enumerate((p0, p1, p2, p3)):
        line_ref[lax.rem(here + distance, 4)] = ref[...]
    branch = jnp.concatenate([line_ref[j] for j in range(4)], axis=1).astype(F32)
    residual = tokens_ref[...].astype(F32) + branch
    residual_ref[...] = residual
    mean = jnp.mean(residual * residual, axis=1, keepdims=True)
    normed = (residual * lax.rsqrt(mean + EPS) * gain_ref[...]).astype(BF16)
    count = outgoing_ref.shape[0]
    slot = iota2((count, residual.shape[0]), 0)
    chooser = ((slot == slots_ref[0:1, :]) | (slot == slots_ref[1:2, :])).astype(F32).astype(BF16)
    outgoing_ref[...] = mm(chooser, normed).astype(BF16)


def route(where, parts, tokens, gain, slots, count):
    vm = pl.BlockSpec(memory_space=pltpu.VMEM)
    return pl.pallas_call(
        route_kernel,
        out_shape=(
            jax.ShapeDtypeStruct(tokens.shape, F32),
            jax.ShapeDtypeStruct((count, tokens.shape[1]), BF16),
        ),
        in_specs=[pl.BlockSpec(memory_space=pltpu.SMEM)] + [vm] * 7,
        out_specs=(vm, vm),
        scratch_shapes=[pltpu.VMEM((4,) + parts[0].shape, BF16)],
        name="route",
    )(where, *parts, tokens, gain, slots)


def expert_kernel(rows_ref, w_hbm, out_ref, sum_ref, w_ref, sem):
    count, _, _, part = w_hbm.shape
    pair = 2

    def fetch(i):
        return pltpu.make_async_copy(w_hbm.at[i], w_ref.at[i], sem.at[i])

    for i in range(count):
        fetch(i).start()
    sum_ref[...] = jnp.zeros_like(sum_ref)
    rows = rows_ref[...]

    def step(s, carry):
        slices = [s * pair + i for i in range(pair)]
        for i in slices:
            fetch(i).wait()
        both = mm(rows, jnp.concatenate([w_ref[i, 0] for i in slices] + [w_ref[i, 1] for i in slices], axis=1))
        gate = both[:, :pair * part]
        hidden = (gate / (1.0 + jnp.exp(-gate)) * both[:, pair * part:]).astype(BF16)
        sum_ref[...] += mm_nt(hidden, jnp.concatenate([w_ref[i, 2] for i in slices], axis=1))
        return carry

    lax.fori_loop(0, count // pair, step, 0)
    out_ref[...] = sum_ref[...].astype(BF16)


def run_expert(rows, weights):
    vm = pl.BlockSpec(memory_space=pltpu.VMEM)
    return pl.pallas_call(
        expert_kernel,
        out_shape=jax.ShapeDtypeStruct(rows.shape, BF16),
        in_specs=[vm, pl.BlockSpec(memory_space=pl.ANY)],
        out_specs=vm,
        scratch_shapes=[
            pltpu.VMEM(rows.shape, F32),
            pltpu.VMEM(weights.shape, BF16),
            pltpu.SemaphoreType.DMA((weights.shape[0],)),
        ],
        name="run_expert",
    )(rows, weights)


def pack_kernel(a_ref, b_ref, c_ref, out_ref, held_ref, in_sem, out_sem):
    refs = (a_ref, b_ref, c_ref)
    inward = [pltpu.make_async_copy(ref.at[0], held_ref.at[i], in_sem.at[i]) for i, ref in enumerate(refs)]
    outward = [pltpu.make_async_copy(held_ref.at[i], out_ref.at[i], out_sem.at[i]) for i in range(3)]
    for copy in inward:
        copy.start()
    for one, other in zip(inward, outward):
        one.wait()
        other.start()
    for copy in outward:
        copy.wait()


def pack(a, b, c):
    anywhere = pl.BlockSpec(memory_space=pl.ANY)
    shape = (3,) + a.shape[1:]
    return pl.pallas_call(
        pack_kernel,
        out_shape=jax.ShapeDtypeStruct(shape, BF16),
        in_specs=[anywhere] * 3,
        out_specs=anywhere,
        scratch_shapes=[pltpu.VMEM(shape, BF16), pltpu.SemaphoreType.DMA((3,)), pltpu.SemaphoreType.DMA((3,))],
        name="pack",
    )(a, b, c)


def finish_kernel(residual_ref, rows_ref, slots_ref, weight_ref, out_ref):
    tokens = residual_ref.shape[0]
    count = rows_ref.shape[0]
    slot = iota2((tokens, count), 1)
    chosen = jnp.where(slot == slots_ref[:, 0:1], weight_ref[:, 0:1], 0.0) + jnp.where(
        slot == slots_ref[:, 1:2], weight_ref[:, 1:2], 0.0
    )
    high = chosen.astype(BF16)
    low = (chosen - high.astype(F32)).astype(BF16)
    rows = rows_ref[...]
    out_ref[...] = (residual_ref[...] + (mm(high, rows) + mm(low, rows))).astype(BF16)


def finish(residual, rows, slots, weight):
    vm = pl.BlockSpec(memory_space=pltpu.VMEM)
    return pl.pallas_call(
        finish_kernel,
        out_shape=jax.ShapeDtypeStruct(residual.shape, BF16),
        in_specs=[vm] * 4,
        out_specs=vm,
        name="finish",
    )(residual, rows, slots, weight)


def shifted(xs, axis):
    size = lax.axis_size(axis)
    return [lax.ppermute(x, axis, [(i, (i + d) % size) for i in range(size)]) for d, x in enumerate(xs, 1)]


def around(x, axis):
    return shifted([x] * (lax.axis_size(axis) - 1), axis)


def shards(
    query_vectors, key_vectors, value_vectors, out_gate, decay_rate, decay_pre, decay_shock, beta_pre,
    head_gain, w_out, tokens, norm_gain, experts_pick, pair_logits, group_logits,
    expert_gate, expert_up, expert_down,
):
    length, _, dh = query_vectors.shape
    chunks = length // CHUNK
    at_x = lax.axis_index("sp_1")
    at_y = lax.axis_index("sp_0")
    where = jnp.stack([at_x, at_y]).astype(jnp.int32)

    expert_all = lax.all_gather(pack(expert_gate, expert_up, expert_down), "tp", axis=0)

    local_rows = tokens.shape[0]
    group_count = group_logits.shape[1]
    group_exp = jnp.exp(group_logits)
    group_share = group_exp / jnp.sum(group_exp, axis=-1, keepdims=True)
    group_index_of = experts_pick[:, 0] // GROUP_SIZE
    group_weight = jnp.sum(
        jnp.where(jnp.arange(group_count)[None, :] == group_index_of[:, None], group_share, 0.0), axis=1
    )
    pair_exp = jnp.exp(pair_logits)
    route_weight = pair_exp / jnp.sum(pair_exp, axis=-1, keepdims=True) * group_weight[:, None]
    capacity = local_rows // group_count
    expert_count = lax.axis_size(SP)
    expert_marks = jnp.sum(
        (experts_pick[:, :, None] == jnp.arange(expert_count, dtype=jnp.int32)[None, None, :]).astype(jnp.int32),
        axis=1,
    )
    before_me = (jnp.arange(local_rows)[None, :] < jnp.arange(local_rows)[:, None]).astype(BF16)
    earlier = jnp.dot(before_me, expert_marks.astype(BF16), preferred_element_type=F32).astype(jnp.int32)
    slot_in = jnp.sum(
        jnp.where(
            experts_pick[:, :, None] == jnp.arange(expert_count, dtype=jnp.int32)[None, None, :],
            earlier[:, None, :], 0,
        ),
        axis=2,
    )
    slot_place = experts_pick * capacity + slot_in

    local, reach, maps = local_attention(
        query_vectors.reshape(length, dh), key_vectors.reshape(length, dh), value_vectors.reshape(length, dh),
        decay_rate,
        decay_pre.reshape(2 * chunks, CHUNK), decay_shock.reshape(2 * chunks, CHUNK),
        beta_pre.reshape(2 * chunks, CHUNK),
    )
    sixteenth = w_out.shape[1] // lax.axis_size(SP)
    w_out, maps = lax.optimization_barrier((w_out, maps))
    w_part = lax.dynamic_slice_in_dim(w_out, (at_x * lax.axis_size("sp_0") + at_y) * sixteenth, sixteenth, 1)
    w_column = lax.all_gather(w_part, "tp", axis=0, tiled=True)
    before, *sends = compose_line(where, maps, around(maps, "sp_1"))
    mixed = mix_heads(
        where, before, shifted(sends, "sp_0"), local, reach,
        out_gate.reshape(length, dh), head_gain.reshape(1, dh),
    )
    mixed, w_column = lax.optimization_barrier((mixed, w_column))
    w_columns = [w_column] + around(w_column, "sp_0")
    mine = lax.all_to_all(mixed, "tp", split_axis=0, concat_axis=1, tiled=True)
    parts = project(where, [mine] + around(mine, "sp_1"), w_columns)
    size = lax.axis_size("sp_1")
    returned = [parts[0]] + [
        lax.ppermute(parts[d], "sp_1", [(i, (i - d) % size) for i in range(size)]) for d in range(1, size)
    ]
    residual, outgoing = route(
        where, returned, tokens, norm_gain.reshape(1, -1), slot_place.T, expert_count * capacity
    )
    width = outgoing.shape[1]
    outgoing = outgoing.reshape(expert_count, capacity, width)
    arrived = lax.all_to_all(outgoing, SP, split_axis=0, concat_axis=0, tiled=True)
    expert_rows = run_expert(arrived.reshape(expert_count * capacity, width), expert_all)
    expert_rows = expert_rows.reshape(expert_count, capacity, width)
    results = lax.all_to_all(expert_rows, SP, split_axis=0, concat_axis=0, tiled=True)
    return finish(residual, results.reshape(expert_count * capacity, width), slot_place, route_weight)


def solution(mesh):
    finer = Mesh(mesh.devices.reshape(4, 4, mesh.shape["tp"]), ("sp_0", "sp_1", "tp"))
    in_specs = (
        P(SP, "tp", None), P(SP, "tp", None), P(SP, "tp", None), P(SP, "tp", None),
        P(None, "tp"),
        P(None, "tp", SP), P(None, "tp", SP), P(None, "tp", SP),
        P(), P("tp", None), P(SP_TP, None), P(),
        P(SP_TP, None), P(SP_TP, None), P(SP_TP, None),
        P(SP, None, "tp"), P(SP, None, "tp"), P(SP, None, "tp"),
    )
    return jax.shard_map(
        shards, mesh=finer, in_specs=in_specs, out_specs=P(SP_TP, None), check_vma=False
    )
```
